32 devices in a mesh: pp: 2 (over x), fs: 4 (over y, core), tp: 4 (over z).
Axes of the slice: x: 2, y: 2, z: 4, core: 2. Of those that a mesh axis runs over, the one named last changes fastest.
Arguments:
- inputs: bfloat16 [512, 2048], P('pp', ('fs', 'tp')), may hold values from -6 to 6
- norm_gain: bfloat16 [2, 2048], P('pp', ('fs', 'tp')), may hold values from 0.099609375 to 1.8984375
- w_value: bfloat16 [2, 2048, 2048], P('pp', None, ('fs', 'tp')), may hold values from -0.125 to 0.125
- w_gate: bfloat16 [2, 2048, 2048], P('pp', None, ('fs', 'tp')), may hold values from -0.125 to 0.125
- w_taps: bfloat16 [2, 31, 2048], P('pp', None, ('fs', 'tp')), may hold values from -1 to 1
- ln_gain: float32 [2, 2048], P('pp', ('fs', 'tp')), may hold values from 0.1 to 1.9
- ln_shift: float32 [2, 2048], P('pp', ('fs', 'tp')), may hold values from -3 to 3
Outputs:
- outputs: bfloat16 [512, 2048], P('pp', ('fs', 'tp'))
The draws below stay inside these ranges and needn't reach their ends.
All inputs are finite; a program needn't handle non-finite values.
Results may differ from the reference program's by a relative error of at most 0.0085.
Values may be sent and summed in bfloat16 or wider, within the bound.
A program may use at most 64 MiB of HBM per device.

```python
import jax
import jax.numpy as jnp
from jax import lax

D = 2048
CONV_W = 31
LEN = 128
MICRO = 4
SECTIONS = 2
TOKENS = 512


def block_scale(rng, dims, pieces, low, high):
    factor_of, own = 1.0, jax.random.fold_in(rng, 6)
    for axis_at, parts in pieces:
        heights = jnp.exp(jax.random.uniform(jax.random.fold_in(own, axis_at), (parts,), jnp.float32, low / len(pieces), high / len(pieces)))
        factor_of = factor_of * jnp.repeat(heights, dims[axis_at] // parts).reshape([-1 if axis == axis_at else 1 for axis in range(len(dims))])
    return factor_of


def bell_draw(stream_key, dims, width, most, split=(), kind=jnp.bfloat16):
    array = jax.random.normal(stream_key, dims, jnp.float32) * width
    if len(split) > 0:
        array = block_scale(stream_key, dims, split, -0.22, 0.18) * array
    return jnp.clip(array, min=-most, max=most).astype(kind)


def setup_inputs(seed: int = 0) -> dict:
    key_of = jax.random.split(jax.random.key(seed), 8)
    inputs = bell_draw(key_of[0], (TOKENS, D), 1.0, 6.0, ((0, 2), (1, 16)))
    norm_gain = jnp.clip(1.0 + 0.18 * jax.random.normal(key_of[1], (SECTIONS, D), jnp.float32), 0.099609375, 1.8984375).astype(jnp.bfloat16)
    w_value = bell_draw(key_of[2], (SECTIONS, D, D), D ** -0.5, 0.125, ((0, 2), (2, 16)))
    w_gate = bell_draw(key_of[3], (SECTIONS, D, D), D ** -0.5, 0.125, ((0, 2), (2, 16)))
    w_taps = bell_draw(key_of[4], (SECTIONS, CONV_W, D), CONV_W ** -0.5, 1.0, ((0, 2), (2, 16)))
    ln_gain = jnp.clip(1.0 + 0.18 * jax.random.normal(key_of[5], (SECTIONS, D), jnp.float32), 0.1, 1.9)
    ln_shift = bell_draw(key_of[6], (SECTIONS, D), 0.5, 3.0, ((0, 2), (1, 16)), jnp.float32)
    return dict(inputs=inputs, norm_gain=norm_gain, w_value=w_value, w_gate=w_gate, w_taps=w_taps, ln_gain=ln_gain, ln_shift=ln_shift)


def section_layer(stream, params):
    norm_gain, w_value, w_gate, w_taps, ln_gain, ln_shift = params
    stream_f = stream.astype(jnp.float32)
    scale_rows = lax.rsqrt(lax.optimization_barrier(jnp.mean(stream_f * stream_f, axis=-1, keepdims=True)) + 1e-06)
    normed = (stream_f * scale_rows * norm_gain.astype(jnp.float32)).astype(jnp.bfloat16)
    flat = normed.reshape(MICRO * LEN, D)
    value_sum = jnp.dot(flat, w_value, preferred_element_type=jnp.float32).reshape(MICRO, LEN, D)
    gate_sum = jnp.dot(flat, w_gate, preferred_element_type=jnp.float32).reshape(MICRO, LEN, D)
    gated_rows = value_sum * jax.nn.sigmoid(gate_sum)
    padded = jnp.pad(gated_rows, ((0, 0), (CONV_W - 1, 0), (0, 0)))
    tap_weights = w_taps.astype(jnp.float32)
    convolved = jnp.zeros((MICRO, LEN, D), jnp.float32)
    for tap_index in range(CONV_W):
        convolved = convolved + padded[:, tap_index:tap_index + LEN] * tap_weights[tap_index]
    row_mean = lax.optimization_barrier(jnp.mean(convolved, axis=-1, keepdims=True))
    row_var = lax.optimization_barrier(jnp.mean(convolved * convolved, axis=-1, keepdims=True)) - row_mean * row_mean
    normed_conv = (convolved - row_mean) * lax.rsqrt(row_var + 1e-05) * ln_gain + ln_shift
    new_stream = (stream_f + jax.nn.silu(normed_conv)).astype(jnp.bfloat16)
    return (new_stream, None)

def reference(inputs, norm_gain, w_value, w_gate, w_taps, ln_gain, ln_shift):
    stream = inputs.reshape(MICRO, LEN, D)
    stream, unused = lax.scan(section_layer, stream, (norm_gain, w_value, w_gate, w_taps, ln_gain, ln_shift))
    return stream.reshape(MICRO * LEN, D)
```

```python
import functools

import jax
import jax.numpy as jnp
from jax import lax
from jax.experimental import pallas as pl
from jax.experimental.pallas import tpu as pltpu
from jax.sharding import PartitionSpec as P

LEN = 128


norm_eps = 1e-06
layer_eps = 1e-05
MESH = pl.DeviceIdType.MESH


def kernel(
    sizes,
    x_ref,
    gain_ref,
    wv_ref,
    wg_ref,
    taps_ref,
    lgain_ref,
    lshift_ref,
    out_ref,
    gath,
    gains,
    stat,
    hbuf,
    pad,
    taps,
    conv_buf,
    new_buf,
    turn,
    gath_sem,
    gain_sem,
    stat_sem,
    out_sem,
    feed_send,
    relay_send,
    gain_send,
    stat_send,
    next_send,
):
    P_, F, T = sizes
    G = F * T
    k, f, t = lax.axis_index("pp"), lax.axis_index("fs"), lax.axis_index("tp")
    M = gath.shape[0]
    C = x_ref.shape[1]
    D = wv_ref.shape[1]
    own_rows = x_ref.shape[0]
    piece = min(LEN, own_rows)
    per_mb = LEN // piece
    per_owner = own_rows // piece
    me = f * T + t
    ring_t = [lax.rem(t + d, T) for d in range(T)]
    pending = []

    def at(kk, ff, tt):
        return {"pp": kk, "fs": ff, "tp": tt}

    def send(src, dst, s_sem, r_sem, dev, cond=None):
        def make():
            return pltpu.make_async_remote_copy(
                src_ref=src, dst_ref=dst, send_sem=s_sem, recv_sem=r_sem,
                device_id=dev, device_id_type=MESH,
            )

        def go():
            make().start()

        def done():
            make().wait_send()

        if cond is None:
            go()
            pending.append(done)
        else:
            pl.when(cond)(go)
            pending.append(lambda: pl.when(cond)(done))

    def await_bytes(ref, sem):
        pltpu.make_async_copy(ref, ref, sem).wait()

    peers = []
    for df in range(F):
        for dt in range(T):
            if df or dt:
                peers.append(at(k, lax.rem(f + df, F), ring_t[dt]))
    others = []
    for dk in range(1, P_):
        for dt in range(T):
            others.append(at(lax.rem(k + dk, P_), f, ring_t[dt]))
    barrier = pltpu.get_barrier_semaphore()
    for dev in peers + others:
        pl.semaphore_signal(barrier, inc=1, device_id=dev, device_id_type=MESH)
    gains[me] = gain_ref[...].astype(jnp.float32)
    taps[...] = taps_ref[0].astype(jnp.float32)
    pad[0:32, :] = jnp.zeros((32, C), jnp.float32)
    turn[...] = jnp.zeros_like(turn)
    pl.semaphore_wait(barrier, len(peers) + len(others))

    for i in range(per_owner):
        p = k * per_owner + i
        m = lax.div(p, per_mb)
        rows = pl.ds(pl.multiple_of(lax.rem(p, per_mb) * piece, piece), piece)
        src = x_ref.at[pl.ds(i * piece, piece)]
        for dt in list(range(1, T)) + [0]:
            dst = gath.at[m, me, rows]
            sem = gath_sem.at[m, me]
            if dt == 0:
                @pl.when(k == 0)
                def _():
                    pltpu.make_async_copy(src, dst, sem).start()

                send(src, dst, feed_send.at[i, dt], sem, at(0, f, t), k != 0)
            else:
                send(src, dst, feed_send.at[i, dt], sem, at(0, f, ring_t[dt]))
        if i == 0:
            for n, dev in enumerate(peers):
                send(gains.at[me], gains.at[me], gain_send.at[n], gain_sem.at[0], dev)

    bits = []
    b = F // 2
    while b:
        bits.append(b)
        b //= 2

    def relay(m):
        count = 0
        for r in [0] + bits + [r for r in range(1, F) if r not in bits]:
            low = (r & -r) if r else F
            row = f ^ r
            for dt in range(T):
                slot = row * T + ring_t[dt]
                block = gath.at[m, slot]
                await_bytes(block, gath_sem.at[m, slot])
                for b in bits:
                    if b < low:
                        send(block, block, relay_send.at[m, count], gath_sem.at[m, slot], at(k, f ^ b, t))
                        count += 1

    def project(m):
        squares = jnp.zeros((LEN, C), jnp.float32)
        for s in range(G):
            xf = gath[m, s].astype(jnp.float32)
            squares = squares + xf * xf
            hbuf[:, s * C : (s + 1) * C] = (xf * gains[s]).astype(jnp.bfloat16)
        scale = lax.rsqrt(jnp.sum(squares, axis=1, keepdims=True) / D + norm_eps)
        value = jnp.dot(hbuf[...], wv_ref[0], preferred_element_type=jnp.float32) * scale
        gate = jnp.dot(hbuf[...], wg_ref[0], preferred_element_type=jnp.float32) * scale
        pad[32:, :] = value * jax.nn.sigmoid(gate)
        W = taps.shape[0]
        step = 32
        for r0 in range(0, LEN, step):
            acc = jnp.zeros((step, C), jnp.float32)
            for j in range(W):
                o = 32 - (W - 1) + j + r0
                acc = acc + pad[o : o + step, :] * taps[j : j + 1, :]
            conv_buf[m, r0 : r0 + step, :] = acc
        conv = conv_buf[m]
        lane = lax.broadcasted_iota(jnp.int32, (LEN, LEN), 1)
        s1 = jnp.sum(conv, axis=1, keepdims=True)
        s2 = jnp.sum(conv * conv, axis=1, keepdims=True)
        both = jnp.where(lane == 0, s1, jnp.where(lane == 1, s2, 0.0))
        stat[m, me] = both.T[0:2, :]
        for n, dev in enumerate(peers):
            send(stat.at[m, me], stat.at[m, me], stat_send.at[m, n], stat_sem.at[m], dev)

    def finish(m):
        await_bytes(stat.at[m, pl.ds(0, G - 1)], stat_sem.at[m])
        turn[0:2, :] = jnp.sum(stat[m], axis=0)
        cols = turn[...].T
        mu = cols[:, 0:1] / D
        var = cols[:, 1:2] / D - mu * mu
        y = (conv_buf[m] - mu) * lax.rsqrt(var + layer_eps) * lgain_ref[...] + lshift_ref[...]
        new = (gath[m, me].astype(jnp.float32) + y * jax.nn.sigmoid(y)).astype(jnp.bfloat16)
        new_buf[m] = new
        for dt in list(range(1, T)) + [0]:
            if P_ > 1:
                send(
                    new_buf.at[m], gath.at[m, me], next_send.at[m, dt], gath_sem.at[m, me],
                    at(lax.rem(k + 1, P_), f, ring_t[dt]), k < P_ - 1,
                )
        for q in range(per_mb):
            p = m * per_mb + q
            owner, i = p // per_owner, p % per_owner
            rows = pl.ds(i * piece, piece)
            part = pl.ds(q * piece, piece)
            if owner == P_ - 1:
                @pl.when(k == P_ - 1)
                def _():
                    out_ref[rows, :] = new_buf[m, part, :]
            else:
                send(
                    new_buf.at[m, part], out_ref.at[rows], next_send.at[m, q], out_sem.at[i],
                    at(owner, f, t), k == P_ - 1,
                )

    for m in range(M):
        relay(m)
        if m == 0:
            await_bytes(gains.at[pl.ds(0, G - 1)], gain_sem.at[0])
        project(m)
        if m:
            finish(m - 1)
    finish(M - 1)
    if P_ > 1:
        @pl.when(k < P_ - 1)
        def _():
            for i in range(per_owner):
                await_bytes(out_ref.at[pl.ds(i * piece, piece)], out_sem.at[i])
    for done in pending:
        done()


def local(sizes, inputs, norm_gain, w_value, w_gate, w_taps, ln_gain, ln_shift):
    P_, F, T = sizes
    G = F * T
    own_rows, C = inputs.shape
    M = own_rows * P_ // LEN
    piece = min(LEN, own_rows)
    per_owner = own_rows // piece
    per_mb = LEN // piece
    D = w_value.shape[1]
    W = w_taps.shape[1]
    bits = F.bit_length() - 1
    relays = T * (F - 1) if bits else 1
    dma = pltpu.SemaphoreType.DMA
    f32, bf16 = jnp.float32, jnp.bfloat16
    return pl.pallas_call(
        functools.partial(kernel, sizes),
        out_shape=jax.ShapeDtypeStruct((own_rows, C), bf16),
        in_specs=[pl.BlockSpec(memory_space=pltpu.VMEM)] * 7,
        out_specs=pl.BlockSpec(memory_space=pltpu.VMEM),
        scratch_shapes=[
            pltpu.VMEM((M, G, LEN, C), bf16),
            pltpu.VMEM((G, 1, C), f32),
            pltpu.VMEM((M, G, 2, LEN), f32),
            pltpu.VMEM((LEN, D), bf16),
            pltpu.VMEM((LEN + 32, C), f32),
            pltpu.VMEM((W, C), f32),
            pltpu.VMEM((M, LEN, C), f32),
            pltpu.VMEM((M, LEN, C), bf16),
            pltpu.VMEM((LEN, LEN), f32),
            dma((M, G)),
            dma((1,)),
            dma((M,)),
            dma((per_owner,)),
            dma((per_owner, T)),
            dma((M, relays)),
            dma((G - 1,)),
            dma((M, G - 1)),
            dma((M, max(T, per_mb))),
        ],
        compiler_params=pltpu.CompilerParams(collective_id=0, has_side_effects=True),
    )(inputs, norm_gain, w_value, w_gate, w_taps, ln_gain, ln_shift)


def solution(mesh):
    sizes = (mesh.shape["pp"], mesh.shape["fs"], mesh.shape["tp"])
    in_specs = (
        P("pp", ("fs", "tp")),
        P("pp", ("fs", "tp")),
        P("pp", None, ("fs", "tp")),
        P("pp", None, ("fs", "tp")),
        P("pp", None, ("fs", "tp")),
        P("pp", ("fs", "tp")),
        P("pp", ("fs", "tp")),
    )
    out_specs = P("pp", ("fs", "tp"))
    return jax.shard_map(
        functools.partial(local, sizes), mesh=mesh, in_specs=in_specs, out_specs=out_specs,
        check_vma=False,
    )
```

```python
import functools

import jax
import jax.numpy as jnp
from jax import lax
from jax.experimental import pallas as pl
from jax.experimental.pallas import tpu as pltpu
from jax.sharding import PartitionSpec as P

LEN = 128


norm_eps = 1e-06
layer_eps = 1e-05
MESH = pl.DeviceIdType.MESH


def kernel(
    sizes,
    x_hbm,
    gain_hbm,
    wv_hbm,
    wg_hbm,
    taps_hbm,
    lgain_hbm,
    lshift_hbm,
    out_ref,
    x_ref,
    gain_ref,
    wv_ref,
    wg_ref,
    taps_ref,
    lgain_ref,
    lshift_ref,
    load_sem,
    gath,
    gains,
    stat,
    hbuf,
    pad,
    taps,
    conv_buf,
    new_buf,
    turn,
    gath_sem,
    gain_sem,
    stat_sem,
    out_sem,
    feed_send,
    relay_send,
    gain_send,
    stat_send,
    next_send,
    back_send,
):
    P_, F, T = sizes
    G = F * T
    k, f, t = lax.axis_index("pp"), lax.axis_index("fs"), lax.axis_index("tp")
    M = gath.shape[0]
    C = x_ref.shape[1]
    D = wv_ref.shape[1]
    own_rows = x_ref.shape[0]
    piece = min(LEN, own_rows)
    per_mb = LEN // piece
    per_owner = own_rows // piece
    head = pad.shape[0] - LEN
    me = f * T + t
    loads = [
        pltpu.make_async_copy(a, b, load_sem.at[n])
        for n, (a, b) in enumerate(
            [
                (x_hbm, x_ref), (gain_hbm, gain_ref), (wv_hbm, wv_ref), (wg_hbm, wg_ref),
                (taps_hbm, taps_ref), (lgain_hbm, lgain_ref), (lshift_hbm, lshift_ref),
            ]
        )
    ]
    for load in loads:
        load.start()
    if T & (T - 1) == 0:
        to_t = [t] + [t ^ d for d in range(T - 1, 0, -1)]
        from_t = to_t
    else:
        to_t = [lax.rem(t + d, T) for d in range(T)]
        from_t = [lax.rem(t + T - d, T) for d in range(T)]

    def at(kk, ff, tt):
        return {"pp": kk, "fs": ff, "tp": tt}

    def send(src, dst, s_sem, r_sem, dev, cond=None):
        def go():
            pltpu.make_async_remote_copy(
                src_ref=src, dst_ref=dst, send_sem=s_sem, recv_sem=r_sem,
                device_id=dev, device_id_type=MESH,
            ).start()

        if cond is None:
            go()
        else:
            pl.when(cond)(go)

    def await_bytes(ref, sem):
        pltpu.make_async_copy(ref, ref, sem).wait()

    peers = []
    for dt in list(range(1, T)) + [0]:
        for df in range(F):
            if df or dt:
                peers.append(at(k, lax.rem(f + df, F), to_t[dt]))
    others = []
    for dk in range(1, P_):
        for dt in range(T):
            others.append(at(lax.rem(k + dk, P_), f, to_t[dt]))
    barrier = pltpu.get_barrier_semaphore()
    for dev in peers + others:
        pl.semaphore_signal(barrier, inc=1, device_id=dev, device_id_type=MESH)
    for load in loads[:2]:
        load.wait()
    gains[me] = gain_ref[...].astype(jnp.float32)
    pad[0:head, :] = jnp.zeros((head, C), jnp.float32)
    turn[...] = jnp.zeros_like(turn)
    pl.semaphore_wait(barrier, len(peers) + len(others))

    for i in range(per_owner):
        p = k * per_owner + i
        m = lax.div(p, per_mb)
        rows = pl.ds(pl.multiple_of(lax.rem(p, per_mb) * piece, piece), piece)
        src = x_ref.at[pl.ds(i * piece, piece)]
        dst = gath.at[m, me, rows]
        sem = gath_sem.at[m, me]

        @pl.when(k == 0)
        def _():
            pltpu.make_async_copy(src, dst, sem).start()

        send(src, dst, feed_send.at[0], sem, at(0, f, t), k != 0)
        for dt in range(1, T):
            send(src, dst, feed_send.at[1], sem, at(0, f, to_t[dt]))
        if i == 0:
            for dev in peers:
                send(gains.at[me], gains.at[me], gain_send.at[0], gain_sem.at[0], dev)
    for load in loads[2:]:
        load.wait()
    taps[...] = taps_ref[0].astype(jnp.float32)

    bits = []
    b = F // 2
    while b:
        bits.append(b)
        b //= 2

    def relay(m, low):
        for r in range(F):
            if ((r & -r) if r else F) == low:
                for tt in from_t:
                    slot = (f ^ r) * T + tt
                    block = gath.at[m, slot]
                    await_bytes(block, gath_sem.at[m, slot])
                    for b in bits:
                        if b < low:
                            send(block, block, relay_send.at[0], gath_sem.at[m, slot], at(k, f ^ b, t))

    def project(m):
        squares = jnp.zeros((LEN, C), jnp.float32)
        for s in range(G):
            xf = gath[m, s].astype(jnp.float32)
            squares = squares + xf * xf
            hbuf[:, s * C : (s + 1) * C] = (xf * gains[s]).astype(jnp.bfloat16)
        scale = lax.rsqrt(jnp.sum(squares, axis=1, keepdims=True) / D + norm_eps)
        value = jnp.dot(hbuf[...], wv_ref[0], preferred_element_type=jnp.float32) * scale
        gate = jnp.dot(hbuf[...], wg_ref[0], preferred_element_type=jnp.float32) * scale
        pad[head:, :] = value * jax.nn.sigmoid(gate)
        W = taps.shape[0]
        step = 32
        for r0 in range(0, LEN, step):
            acc = jnp.zeros((step, C), jnp.float32)
            for j in range(W):
                o = head - (W - 1) + j + r0
                acc = acc + pad[o : o + step, :] * taps[j : j + 1, :]
            conv_buf[m, r0 : r0 + step, :] = acc
        conv = conv_buf[m]
        lane = lax.broadcasted_iota(jnp.int32, (LEN, LEN), 1)
        s1 = jnp.sum(conv, axis=1, keepdims=True)
        s2 = jnp.sum(conv * conv, axis=1, keepdims=True)
        both = jnp.where(lane == 0, s1, jnp.where(lane == 1, s2, 0.0))
        stat[m, me] = both.T[0:2, :]
        for dev in peers:
            send(stat.at[m, me], stat.at[m, me], stat_send.at[0], stat_sem.at[m], dev)

    def finish(m):
        await_bytes(stat.at[m, pl.ds(0, G - 1)], stat_sem.at[m])
        turn[0:2, :] = jnp.sum(stat[m], axis=0)
        cols = turn[...].T
        mu = cols[:, 0:1] / D
        var = cols[:, 1:2] / D - mu * mu
        y = (conv_buf[m] - mu) * lax.rsqrt(var + layer_eps) * lgain_ref[...] + lshift_ref[...]
        new = (gath[m, me].astype(jnp.float32) + y * jax.nn.sigmoid(y)).astype(jnp.bfloat16)
        new_buf[m] = new
        if P_ > 1:
            for tt in to_t:
                send(
                    new_buf.at[m], gath.at[m, me], next_send.at[0], gath_sem.at[m, me],
                    at(lax.rem(k + 1, P_), f, tt), k < P_ - 1,
                )
        for q in range(per_mb):
            p = m * per_mb + q
            owner, i = p // per_owner, p % per_owner
            rows = pl.ds(i * piece, piece)
            part = pl.ds(q * piece, piece)
            if owner == P_ - 1:
                @pl.when(k == P_ - 1)
                def _():
                    out_ref[rows, :] = new_buf[m, part, :]
            else:
                send(
                    new_buf.at[m, part], out_ref.at[rows], back_send.at[0], out_sem.at[i],
                    at(owner, f, t), k == P_ - 1,
                )

    levels = [F] + bits
    relay(0, F)
    for m in range(M):
        if m + 1 < M:
            relay(m + 1, F)
        for low in levels[1:]:
            relay(m, low)
        if m == 0:
            await_bytes(gains.at[pl.ds(0, G - 1)], gain_sem.at[0])
        project(m)
        if m:
            finish(m - 1)
    await_bytes(gath.at[:, pl.ds(0, T * (F - 1))], relay_send.at[0])
    await_bytes(stat.at[:, pl.ds(0, G - 1)], stat_send.at[0])
    await_bytes(gains.at[pl.ds(0, G - 1)], gain_send.at[0])
    for i in range(per_owner):
        await_bytes(gath.at[0, pl.ds(0, T - 1), pl.ds(0, piece)], feed_send.at[1])
    if P_ > 1:
        @pl.when(k != 0)
        def _():
            await_bytes(x_ref, feed_send.at[0])

    finish(M - 1)
    if P_ > 1:
        @pl.when(k < P_ - 1)
        def _():
            await_bytes(gath.at[:, pl.ds(0, T)], next_send.at[0])
            for i in range(per_owner):
                await_bytes(out_ref.at[pl.ds(i * piece, piece)], out_sem.at[i])

        @pl.when(k == P_ - 1)
        def _():
            for _i in range(per_owner * (P_ - 1)):
                await_bytes(out_ref.at[pl.ds(0, piece)], back_send.at[0])


def local(sizes, inputs, norm_gain, w_value, w_gate, w_taps, ln_gain, ln_shift):
    P_, F, T = sizes
    G = F * T
    own_rows, C = inputs.shape
    M = own_rows * P_ // LEN
    piece = min(LEN, own_rows)
    per_owner = own_rows // piece
    per_mb = LEN // piece
    D = w_value.shape[1]
    W = w_taps.shape[1]
    head = -(-(W - 1) // 8) * 8
    operands = (inputs, norm_gain, w_value, w_gate, w_taps, ln_gain, ln_shift)
    dma = pltpu.SemaphoreType.DMA
    f32, bf16 = jnp.float32, jnp.bfloat16
    return pl.pallas_call(
        functools.partial(kernel, sizes),
        out_shape=jax.ShapeDtypeStruct((own_rows, C), bf16),
        in_specs=[pl.BlockSpec(memory_space=pl.ANY)] * 7,
        out_specs=pl.BlockSpec(memory_space=pltpu.VMEM),
        scratch_shapes=[
            *[pltpu.VMEM(a.shape, a.dtype) for a in operands],
            dma((len(operands),)),
            pltpu.VMEM((M, G, LEN, C), bf16),
            pltpu.VMEM((G, 1, C), f32),
            pltpu.VMEM((M, G, 2, LEN), f32),
            pltpu.VMEM((LEN, D), bf16),
            pltpu.VMEM((LEN + head, C), f32),
            pltpu.VMEM((W, C), f32),
            pltpu.VMEM((M, LEN, C), f32),
            pltpu.VMEM((M, LEN, C), bf16),
            pltpu.VMEM((LEN, LEN), f32),
            dma((M, G)),
            dma((1,)),
            dma((M,)),
            dma((per_owner,)),
            dma((2,)),
            dma((1,)),
            dma((1,)),
            dma((1,)),
            dma((1,)),
            dma((1,)),
        ],
        compiler_params=pltpu.CompilerParams(collective_id=0, has_side_effects=True),
    )(*operands)


def solution(mesh):
    sizes = (mesh.shape["pp"], mesh.shape["fs"], mesh.shape["tp"])
    in_specs = (
        P("pp", ("fs", "tp")),
        P("pp", ("fs", "tp")),
        P("pp", None, ("fs", "tp")),
        P("pp", None, ("fs", "tp")),
        P("pp", None, ("fs", "tp")),
        P("pp", ("fs", "tp")),
        P("pp", ("fs", "tp")),
    )
    out_specs = P("pp", ("fs", "tp"))
    return jax.shard_map(
        functools.partial(local, sizes), mesh=mesh, in_specs=in_specs, out_specs=out_specs,
        check_vma=False,
    )
```

```python
import functools

import jax
import jax.numpy as jnp
from jax import lax
from jax.experimental import pallas as pl
from jax.experimental.pallas import tpu as pltpu
from jax.sharding import PartitionSpec as P

LEN = 128


norm_eps = 1e-06
layer_eps = 1e-05
MESH = pl.DeviceIdType.MESH


def kernel(
    sizes,
    x_hbm,
    gain_hbm,
    wv_hbm,
    wg_hbm,
    taps_hbm,
    lgain_hbm,
    lshift_hbm,
    out_ref,
    x_ref,
    gain_ref,
    wv_ref,
    wg_ref,
    taps_ref,
    lgain_ref,
    lshift_ref,
    load_sem,
    gath,
    gains,
    stat,
    hbuf,
    pad,
    taps,
    conv_buf,
    new_buf,
    turn,
    gath_sem,
    gain_sem,
    stat_sem,
    out_sem,
    feed_send,
    relay_send,
    gain_send,
    stat_send,
    next_send,
    back_send,
):
    P_, F, T = sizes
    G = F * T
    k, f, t = lax.axis_index("pp"), lax.axis_index("fs"), lax.axis_index("tp")
    M = gath.shape[0]
    C = x_ref.shape[1]
    D = wv_ref.shape[1]
    own_rows = x_ref.shape[0]
    piece = min(LEN, own_rows)
    per_mb = LEN // piece
    per_owner = own_rows // piece
    head = pad.shape[0] - LEN
    me = f * T + t
    loads = [
        pltpu.make_async_copy(a, b, load_sem.at[n])
        for n, (a, b) in enumerate(
            [
                (x_hbm, x_ref), (gain_hbm, gain_ref), (wv_hbm, wv_ref), (wg_hbm, wg_ref),
                (taps_hbm, taps_ref), (lgain_hbm, lgain_ref), (lshift_hbm, lshift_ref),
            ]
        )
    ]
    for load in loads:
        load.start()
    if T & (T - 1) == 0:
        to_t = [t] + [t ^ d for d in range(T - 1, 0, -1)]
        from_t = to_t
    else:
        to_t = [lax.rem(t + d, T) for d in range(T)]
        from_t = [lax.rem(t + T - d, T) for d in range(T)]

    def at(kk, ff, tt):
        return {"pp": kk, "fs": ff, "tp": tt}

    def send(src, dst, s_sem, r_sem, dev, cond=None):
        def go():
            pltpu.make_async_remote_copy(
                src_ref=src, dst_ref=dst, send_sem=s_sem, recv_sem=r_sem,
                device_id=dev, device_id_type=MESH,
            ).start()

        if cond is None:
            go()
        else:
            pl.when(cond)(go)

    def await_bytes(ref, sem):
        pltpu.make_async_copy(ref, ref, sem).wait()

    peers = []
    for dt in list(range(1, T)) + [0]:
        for df in range(F):
            if df or dt:
                peers.append(at(k, lax.rem(f + df, F), to_t[dt]))
    others = []
    for dk in range(1, P_):
        for dt in range(T):
            others.append(at(lax.rem(k + dk, P_), f, to_t[dt]))
    barrier = pltpu.get_barrier_semaphore()
    for dev in peers + others:
        pl.semaphore_signal(barrier, inc=1, device_id=dev, device_id_type=MESH)
    for load in loads[:2]:
        load.wait()
    gains[me] = gain_ref[...].astype(jnp.float32)
    pad[0:head, :] = jnp.zeros((head, C), jnp.float32)
    turn[...] = jnp.zeros_like(turn)
    pl.semaphore_wait(barrier, len(peers) + len(others))

    for i in range(per_owner):
        p = k * per_owner + i
        m = lax.div(p, per_mb)
        rows = pl.ds(pl.multiple_of(lax.rem(p, per_mb) * piece, piece), piece)
        src = x_ref.at[pl.ds(i * piece, piece)]
        dst = gath.at[m, me, rows]
        sem = gath_sem.at[m, me]

        @pl.when(k == 0)
        def _():
            pltpu.make_async_copy(src, dst, sem).start()

        send(src, dst, feed_send.at[0], sem, at(0, f, t), k != 0)
        for dt in range(1, T):
            send(src, dst, feed_send.at[1], sem, at(0, f, to_t[dt]))
        if i == 0:
            for dev in peers:
                send(gains.at[me], gains.at[me], gain_send.at[0], gain_sem.at[0], dev)
    for load in loads[2:]:
        load.wait()
    taps[...] = taps_ref[0].astype(jnp.float32)

    bits = []
    b = F // 2
    while b:
        bits.append(b)
        b //= 2

    def relay(m, low):
        for r in range(F):
            if ((r & -r) if r else F) == low:
                for tt in from_t:
                    slot = (f ^ r) * T + tt
                    block = gath.at[m, slot]
                    await_bytes(block, gath_sem.at[m, slot])
                    for b in bits:
                        if b < low:
                            send(block, block, relay_send.at[0], gath_sem.at[m, slot], at(k, f ^ b, t))

    def project(m):
        squares = jnp.zeros((LEN, C), jnp.float32)
        for s in range(G):
            xf = gath[m, s].astype(jnp.float32)
            squares = squares + xf * xf
            hbuf[:, s * C : (s + 1) * C] = (xf * gains[s]).astype(jnp.bfloat16)
        scale = lax.rsqrt(jnp.sum(squares, axis=1, keepdims=True) / D + norm_eps)
        value = jnp.dot(hbuf[...], wv_ref[0], preferred_element_type=jnp.float32) * scale
        gate = jnp.dot(hbuf[...], wg_ref[0], preferred_element_type=jnp.float32) * scale
        pad[head:, :] = value * jax.nn.sigmoid(gate)
        W = taps.shape[0]
        step = 32
        for r0 in range(0, LEN, step):
            acc = jnp.zeros((step, C), jnp.float32)
            for j in range(W):
                o = head - (W - 1) + j + r0
                acc = acc + pad[o : o + step, :] * taps[j : j + 1, :]
            conv_buf[m, r0 : r0 + step, :] = acc
        conv = conv_buf[m]
        lane = lax.broadcasted_iota(jnp.int32, (LEN, LEN), 1)
        s1 = jnp.sum(conv, axis=1, keepdims=True)
        s2 = jnp.sum(conv * conv, axis=1, keepdims=True)
        both = jnp.where(lane == 0, s1, jnp.where(lane == 1, s2, 0.0))
        stat[m, me] = both.T[0:2, :]
        for dev in peers:
            send(stat.at[m, me], stat.at[m, me], stat_send.at[0], stat_sem.at[m], dev)

    def finish(m):
        await_bytes(stat.at[m, pl.ds(0, G - 1)], stat_sem.at[m])
        turn[0:2, :] = jnp.sum(stat[m], axis=0)
        cols = turn[...].T
        mu = cols[:, 0:1] / D
        var = cols[:, 1:2] / D - mu * mu
        y = (conv_buf[m] - mu) * lax.rsqrt(var + layer_eps) * lgain_ref[...] + lshift_ref[...]
        new = (gath[m, me].astype(jnp.float32) + y * jax.nn.sigmoid(y)).astype(jnp.bfloat16)
        new_buf[m] = new
        if P_ > 1:
            for tt in to_t:
                send(
                    new_buf.at[m], gath.at[m, me], next_send.at[0], gath_sem.at[m, me],
                    at(lax.rem(k + 1, P_), f, tt), k < P_ - 1,
                )
        for q in range(per_mb):
            p = m * per_mb + q
            owner, i = p // per_owner, p % per_owner
            rows = pl.ds(i * piece, piece)
            part = pl.ds(q * piece, piece)
            if owner == P_ - 1:
                @pl.when(k == P_ - 1)
                def _():
                    out_ref[rows, :] = new_buf[m, part, :]
            else:
                send(
                    new_buf.at[m, part], out_ref.at[rows], back_send.at[0], out_sem.at[i],
                    at(owner, f, t), k == P_ - 1,
                )

    levels = [F] + bits

    def run(ahead, lag):
        for m in range(min(ahead, M)):
            relay(m, F)
        for m in range(M):
            if ahead == 1 and m + 1 < M:
                relay(m + 1, F)
            for low in levels[1:-1]:
                relay(m, low)
            if ahead > 1 and m + ahead < M:
                relay(m + ahead, F)
            if lag > 1 and m > 1:
                finish(m - 2)
            if len(levels) > 1:
                relay(m, levels[-1])
            if m == 0:
                await_bytes(gains.at[pl.ds(0, G - 1)], gain_sem.at[0])
            project(m)
            if lag == 1 and m:
                finish(m - 1)
        if lag > 1 and M > 1:
            finish(M - 2)

    if P_ == 1:
        run(2, 1)
    else:
        pl.when(k == 0)(lambda: run(1, 1))
        pl.when(k != 0)(lambda: run(1, 2))
    await_bytes(gath.at[:, pl.ds(0, T * (F - 1))], relay_send.at[0])
    await_bytes(stat.at[:, pl.ds(0, G - 1)], stat_send.at[0])
    await_bytes(gains.at[pl.ds(0, G - 1)], gain_send.at[0])
    for i in range(per_owner):
        await_bytes(gath.at[0, pl.ds(0, T - 1), pl.ds(0, piece)], feed_send.at[1])
    if P_ > 1:
        @pl.when(k != 0)
        def _():
            await_bytes(x_ref, feed_send.at[0])

    finish(M - 1)
    if P_ > 1:
        @pl.when(k < P_ - 1)
        def _():
            await_bytes(gath.at[:, pl.ds(0, T)], next_send.at[0])
            for i in range(per_owner):
                await_bytes(out_ref.at[pl.ds(i * piece, piece)], out_sem.at[i])

        @pl.when(k == P_ - 1)
        def _():
            for _i in range(per_owner * (P_ - 1)):
                await_bytes(out_ref.at[pl.ds(0, piece)], back_send.at[0])


def local(sizes, inputs, norm_gain, w_value, w_gate, w_taps, ln_gain, ln_shift):
    P_, F, T = sizes
    G = F * T
    own_rows, C = inputs.shape
    M = own_rows * P_ // LEN
    piece = min(LEN, own_rows)
    per_owner = own_rows // piece
    per_mb = LEN // piece
    D = w_value.shape[1]
    W = w_taps.shape[1]
    head = -(-(W - 1) // 8) * 8
    operands = (inputs, norm_gain, w_value, w_gate, w_taps, ln_gain, ln_shift)
    dma = pltpu.SemaphoreType.DMA
    f32, bf16 = jnp.float32, jnp.bfloat16
    return pl.pallas_call(
        functools.partial(kernel, sizes),
        out_shape=jax.ShapeDtypeStruct((own_rows, C), bf16),
        in_specs=[pl.BlockSpec(memory_space=pl.ANY)] * 7,
        out_specs=pl.BlockSpec(memory_space=pltpu.VMEM),
        scratch_shapes=[
            *[pltpu.VMEM(a.shape, a.dtype) for a in operands],
            dma((len(operands),)),
            pltpu.VMEM((M, G, LEN, C), bf16),
            pltpu.VMEM((G, 1, C), f32),
            pltpu.VMEM((M, G, 2, LEN), f32),
            pltpu.VMEM((LEN, D), bf16),
            pltpu.VMEM((LEN + head, C), f32),
            pltpu.VMEM((W, C), f32),
            pltpu.VMEM((M, LEN, C), f32),
            pltpu.VMEM((M, LEN, C), bf16),
            pltpu.VMEM((LEN, LEN), f32),
            dma((M, G)),
            dma((1,)),
            dma((M,)),
            dma((per_owner,)),
            dma((2,)),
            dma((1,)),
            dma((1,)),
            dma((1,)),
            dma((1,)),
            dma((1,)),
        ],
        compiler_params=pltpu.CompilerParams(collective_id=0, has_side_effects=True),
    )(*operands)


def solution(mesh):
    sizes = (mesh.shape["pp"], mesh.shape["fs"], mesh.shape["tp"])
    in_specs = (
        P("pp", ("fs", "tp")),
        P("pp", ("fs", "tp")),
        P("pp", None, ("fs", "tp")),
        P("pp", None, ("fs", "tp")),
        P("pp", None, ("fs", "tp")),
        P("pp", ("fs", "tp")),
        P("pp", ("fs", "tp")),
    )
    out_specs = P("pp", ("fs", "tp"))
    return jax.shard_map(
        functools.partial(local, sizes), mesh=mesh, in_specs=in_specs, out_specs=out_specs,
        check_vma=False,
    )
```
